128 devices in a mesh: sp: 64 (over z, y, x), tp: 2 (over core).
Axes of the slice: x: 4, y: 4, z: 4, core: 2. Of those that a mesh axis runs over, the one named last changes fastest.
Arguments:
- mid_rows: bfloat16 [16384, 2048], P(('sp', 'tp')), may hold values from -6 to 6
- cotangent: bfloat16 [16384, 2048], P(('sp', 'tp')), may hold values from -24 to 24
- routes: int32 [16384, 2], P(('sp', 'tp')), may hold values from 0 to 63, all different within a row; in each aligned block of 128 rows (0 to 127, 128 to 255, ...) at most 8 rows name the same one
- route_weight: float32 [16384, 2], P(('sp', 'tp')), may hold values from 0.3 to 2
- filtered: bfloat16 [16384, 2048], P('sp', 'tp'), may hold values from -30 to 30
- conv_taps: float32 [31, 2048], P(None, 'tp'), may hold values from -1 to 1
- norm_gain: float32 [2048], P('tp'), may hold values from 0.1 to 1.9
- out_weight: bfloat16 [2048, 2048], P('tp'), may hold values from -0.125 to 0.125
- gate_weight: bfloat16 [64, 2048, 1024], P('sp', None, 'tp'), may hold values from -0.125 to 0.125
- up_weight: bfloat16 [64, 2048, 1024], P('sp', None, 'tp'), may hold values from -0.125 to 0.125
- down_weight: bfloat16 [64, 1024, 2048], P('sp', 'tp'), may hold values from -0.1875 to 0.1875
Outputs:
- gate_grad: float32 [64, 2048, 1024], P('sp', None, 'tp')
- up_grad: float32 [64, 2048, 1024], P('sp', None, 'tp')
- down_grad: float32 [64, 1024, 2048], P('sp', 'tp')
- proj_grad: float32 [2048, 2048], P('sp', 'tp')
- input_grad: bfloat16 [16384, 2048], P('sp', 'tp')
The draws below stay inside these ranges and needn't reach their ends.
Inputs may be any that keep to these rules, and one draw needn't show every extreme that they name: `routes`: each row names 2 different experts. In each aligned block of 128 rows no expert is named by more than 8 rows.
All inputs are finite; a program needn't handle non-finite values.
Results may differ from the reference program's by a relative error of at most 0.0075.
Values may be sent and summed in bfloat16 or wider, within the bound.
A program may use at most 128 MiB of HBM per device.

```python
import math
import jax
import jax.numpy as jnp
import numpy as np
from jax import lax

D = 2048
FFE = 1024
TAPS = 31
TOPK = 2
EXPERTS = 64
TOKENS = 16384
ROWS_DEV = 128
CAP = 8
N_SP = 64
N_TP = 2


def draw_filtered(key, part):
    base_key, chan_key, row_key = jax.random.split(key, 3)
    channel = jnp.arange(D)
    block_factor = jnp.where(channel >= D // 2, 3.0, 1.0)
    spread = jnp.exp(jax.random.uniform(chan_key, (D,), jnp.float32, -0.7, 0.7))
    values = jnp.clip(jax.random.normal(base_key, (TOKENS, D), jnp.float32), -4.0, 4.0)
    return (values * block_factor * spread).astype(jnp.bfloat16)


def raised(values, own_key, source, target, shards_of, factor):
    def block_of(dim):
        return (jnp.arange(values.shape[dim]) // (values.shape[dim] // shards_of)).reshape((-1,) + (1,) * (values.ndim - 1 - dim))

    one_side = jax.random.permutation(own_key, shards_of)[block_of(target)]
    second = (block_of(target) + shards_of // 2) % shards_of
    return jnp.where((block_of(source) == one_side) | (block_of(source) == second), factor * values, values)


def block_levels(own_key, extent, cuts, smallest, top_value):
    gain, own = 1.0, jax.random.fold_in(own_key, 6)
    for axis_at, blocks in cuts:
        steps = jnp.exp(jax.random.uniform(jax.random.fold_in(own, axis_at), (blocks,), jnp.float32, smallest / len(cuts), top_value / len(cuts)))
        gain = gain * jnp.repeat(steps, extent[axis_at] // blocks).reshape([-1 if axis == axis_at else 1 for axis in range(len(extent))])
    return gain


def deal_out(stream_key, own, number, rows, count, top, limit, lean):
    sequence = jax.random.permutation(stream_key, count)
    heavy_load, common = portions_of(count, rows * top, limit, lean, True), portions_of(count, rows * top, limit, lean, False)
    places = jnp.arange(count)

    def named(lengths, offset_by):
        used = int((lengths > 0).sum())
        fixed = max(1, used // 4)
        moved = fixed + (places - fixed + offset_by * (used - fixed)) % max(1, count - fixed)
        return jnp.zeros((count,), jnp.int32).at[sequence[jnp.where(places < fixed, places, moved)]].set(jnp.asarray(lengths, jnp.int32))

    lengths = jnp.where(number % 4 == 0, named(heavy_load, number // 4), named(common, number - number // 4 - 1))
    mixed = jax.random.permutation(jax.random.fold_in(own, 3), count)
    source_of, taker = mixed[0:count // 2 * 2:2], mixed[1:count // 2 * 2:2]
    slack = jnp.minimum(lengths[source_of] - 1, limit - lengths[taker]) // 2
    slack = jnp.where((source_of == sequence[0]) | (taker == sequence[0]) | (lengths[taker] == 0), 0, jnp.maximum(slack, 0))
    moved = jax.random.randint(jax.random.fold_in(own, 4), (count // 2,), 0, 1 << 20) % (slack + 1)
    lengths = lengths.at[source_of].add(-moved).at[taker].add(moved)
    labels = jnp.searchsorted(jnp.cumsum(lengths), jnp.arange(rows * top), side="right").astype(jnp.int32)
    grid = labels.reshape(top, rows).T
    grid = grid[jax.random.permutation(jax.random.fold_in(own, 1), rows)]
    offset_by = jax.random.randint(jax.random.fold_in(own, 2), (rows, 1), 0, top)
    return jnp.take_along_axis(grid, (jnp.arange(top)[None, :] + offset_by) % top, axis=1)


def portions_of(number_of, total, bound, skew, full):
    weights = [(1 << 20) // math.isqrt(rank ** skew) + 1 for rank in range(1, number_of + 1)]
    largest = bound if full else min(bound, max(-(-total // number_of), total * weights[0] // sum(weights)))
    least = 1 if total - largest >= number_of - 1 else 0
    holding, rest = [largest] + [least] * (number_of - 1), total - largest - least * (number_of - 1)
    while rest > 0:
        candidates = [i for i in range(1, number_of) if holding[i] < largest] or [i for i in range(1, number_of) if holding[i] < bound]
        pool, budget = sum([weights[i] for i in candidates]), rest
        for i in candidates:
            addition = min(bound - holding[i], max(1, budget * weights[i] // pool), rest)
            holding[i] = holding[i] + addition
            rest = rest - addition
    return np.array(holding)


def gaussian(rng, shape, scale, limit, cuts=(), kind=jnp.bfloat16):
    level = block_levels(rng, shape, cuts, -0.22, 0.18) if cuts else 1.0
    values = jax.random.normal(rng, shape, jnp.float32) * scale * level
    return jnp.minimum(jnp.maximum(values, -limit), limit).astype(kind)


def bell_draw_with(key, dims, deviation, bound, cuts, heavy, kind=jnp.bfloat16):
    values = deviation * jax.random.normal(key, dims, jnp.float32)
    if cuts:
        values = values * block_levels(key, dims, cuts, -0.22, 0.18)
    return jnp.clip(raised(values, jax.random.fold_in(key, 3), *heavy), -bound, bound).astype(kind)


def setup_inputs(seed: int = 0) -> dict:
    keys = jax.random.split(jax.random.key(seed), 12)
    mid_rows = gaussian(keys[0], (TOKENS, D), 1.0, 6.0, ((0, 128),))
    cotangent = bell_draw_with(keys[1], (TOKENS, D), 1.0, 24.0, ((0, 128),), (0, 1, 128, 5.5))
    routes_keys = jax.random.split(jax.random.fold_in(keys[2], 1), TOKENS // ROWS_DEV)
    routes_turns = jax.random.permutation(jax.random.fold_in(keys[2], 3), TOKENS // ROWS_DEV)
    routes = jax.vmap(lambda own, number: deal_out(jax.random.fold_in(keys[2], 2), own, number, ROWS_DEV, EXPERTS, TOPK, CAP, 2))(routes_keys, routes_turns).reshape((TOKENS, TOPK))
    route_weight = jnp.clip(jnp.exp(math.log(2.0) - 1.89712 * jax.random.uniform(keys[3], (TOKENS, TOPK), jnp.float32) ** block_levels(keys[3], (TOKENS, TOPK), ((0, 128),), -0.2, 0.2)), 0.3, 2.0)
    filtered = draw_filtered(jax.random.fold_in(keys[11], 71), 0)
    conv_taps = gaussian(keys[5], (TAPS, D), TAPS ** -0.5, 1.0, ((1, 2),), jnp.float32)
    norm_gain = jnp.clip(1.0 + 0.18 * jax.random.normal(keys[6], (D,), jnp.float32), 0.1, 1.9)
    out_weight = gaussian(keys[7], (D, D), D ** -0.5, 0.125, ((0, 2),))
    gate_weight = gaussian(keys[8], (EXPERTS, D, FFE), D ** -0.5, 0.125, ((0, 64), (2, 2)))
    up_weight = gaussian(keys[9], (EXPERTS, D, FFE), D ** -0.5, 0.125, ((0, 64), (2, 2)))
    down_weight = gaussian(keys[10], (EXPERTS, FFE, D), FFE ** -0.5, 0.1875, ((0, 64), (1, 2)))
    return dict(mid_rows=mid_rows, cotangent=cotangent, routes=routes, route_weight=route_weight, filtered=filtered, conv_taps=conv_taps, norm_gain=norm_gain, out_weight=out_weight, gate_weight=gate_weight, up_weight=up_weight, down_weight=down_weight)


NORM_EPS = 1e-05

def silu_grad(pre_act):
    logistic = jax.nn.sigmoid(pre_act)
    return logistic * (1.0 + pre_act * (1.0 - logistic))

def reference(mid_rows, cotangent, routes, route_weight, filtered, conv_taps, norm_gain, out_weight, gate_weight, up_weight, down_weight):
    total_routes = TOKENS * TOPK
    flattened = routes.reshape(total_routes)
    weight_flat = jnp.concatenate([route_weight.reshape(total_routes), jnp.zeros((1,), jnp.float32)])
    route_ids = jnp.arange(total_routes, dtype=jnp.int32)
    slot_total = N_SP * N_TP * CAP
    half_width = FFE // N_TP

    def expert_step(collected, expert):
        chosen = flattened == expert
        positions = jnp.cumsum(chosen.astype(jnp.int32)) - 1
        target = jnp.where(chosen, positions, slot_total).astype(jnp.int32)
        slot_owner = jnp.full((slot_total + 1,), total_routes, jnp.int32).at[target].set(route_ids)[:slot_total]
        token_of = (slot_owner // TOPK).astype(jnp.int32)
        inputs = jnp.take(mid_rows, token_of, axis=0, mode='fill', fill_value=0)
        cot_rows = jnp.take(cotangent, token_of, axis=0, mode='fill', fill_value=0).astype(jnp.float32)
        route_scale = weight_flat[slot_owner]
        routed = (route_scale[:, None] * cot_rows).astype(jnp.bfloat16)
        gate_mat = gate_weight[expert]
        up_mat = up_weight[expert]
        down_mat = down_weight[expert]
        pre_gate = jnp.dot(inputs, gate_mat, preferred_element_type=jnp.float32)
        pre_up = jnp.dot(inputs, up_mat, preferred_element_type=jnp.float32)
        gate_act = jax.nn.silu(pre_gate)
        hidden = (gate_act * pre_up).astype(jnp.bfloat16)
        down_part = jnp.dot(hidden.T, routed, preferred_element_type=jnp.float32)
        hidden_grad = jnp.dot(routed, down_mat.T, preferred_element_type=jnp.float32)
        gate_pre = (hidden_grad * pre_up * silu_grad(pre_gate)).astype(jnp.bfloat16)
        up_pre = (hidden_grad * gate_act).astype(jnp.bfloat16)
        gate_part = jnp.dot(inputs.T, gate_pre, preferred_element_type=jnp.float32)
        up_part = jnp.dot(inputs.T, up_pre, preferred_element_type=jnp.float32)
        summed = jnp.zeros((slot_total, D), jnp.float32)
        for band_index in range(N_TP):
            band_start = band_index * half_width
            band_stop = band_start + half_width
            band_term = jnp.dot(gate_pre[:, band_start:band_stop], gate_mat[:, band_start:band_stop].T, preferred_element_type=jnp.float32)
            band_term = band_term + jnp.dot(up_pre[:, band_start:band_stop], up_mat[:, band_start:band_stop].T, preferred_element_type=jnp.float32)
            summed = summed + lax.optimization_barrier(band_term.astype(jnp.bfloat16)).astype(jnp.float32)
        route_grad = summed.astype(jnp.bfloat16)
        collected = collected.at[slot_owner].set(route_grad)
        return (collected, (gate_part, up_part, down_part))
    start_rows = jnp.zeros((total_routes + 1, D), jnp.bfloat16)
    collected, (gate_grad, up_grad, down_grad) = lax.scan(expert_step, start_rows, jnp.arange(EXPERTS, dtype=jnp.int32))
    route_sum = lax.optimization_barrier(jnp.sum(collected[:total_routes].astype(jnp.float32).reshape(TOKENS, TOPK, D), axis=1))
    mid_grad = (cotangent.astype(jnp.float32) + route_sum).astype(jnp.bfloat16)
    values = filtered.astype(jnp.float32)
    average = lax.optimization_barrier(jnp.mean(values, axis=1, keepdims=True))
    variance = lax.optimization_barrier(jnp.mean(values * values, axis=1, keepdims=True)) - average * average
    inv_scale = lax.rsqrt(variance + NORM_EPS)
    normed = (values - average) * inv_scale
    scaled = normed * norm_gain
    activated = jax.nn.silu(scaled).astype(jnp.bfloat16)
    proj_grad = jnp.dot(mid_grad.T, activated, preferred_element_type=jnp.float32)
    act_grad = jnp.dot(mid_grad, out_weight.T, preferred_element_type=jnp.float32)
    scaled_grad = act_grad * silu_grad(scaled) * norm_gain
    grad_mean = lax.optimization_barrier(jnp.mean(scaled_grad, axis=1, keepdims=True))
    grad_corr = lax.optimization_barrier(jnp.mean(scaled_grad * normed, axis=1, keepdims=True))
    conv_grad = (inv_scale * (scaled_grad - grad_mean - normed * grad_corr)).astype(jnp.bfloat16)
    halo_width = TAPS // 2
    padded = jnp.pad(conv_grad, ((halo_width, halo_width), (0, 0))).astype(jnp.float32)
    accumulated = jnp.zeros((TOKENS, D), jnp.float32)
    for offset in range(TAPS):
        lead = 2 * halo_width - offset
        accumulated = accumulated + conv_taps[offset] * padded[lead:lead + TOKENS]
    input_grad = accumulated.astype(jnp.bfloat16)
    return (gate_grad, up_grad, down_grad, proj_grad, input_grad)
```

```python
import jax
import jax.numpy as jnp
from jax import lax
from jax.sharding import Mesh
from jax.sharding import PartitionSpec as P

SP = ("sp_0", "sp_1", "sp_2")
SP_TP = ("sp_0", "sp_1", "sp_2", "tp")
NORM_EPS = 1e-05
CAPACITY = 8
SWAP = [(0, 1), (1, 0)]


def dot_f32(a, b, dims):
    return lax.dot_general(a, b, (dims, ((), ())), preferred_element_type=jnp.float32)


def silu_grad(pre_act):
    logistic = jax.nn.sigmoid(pre_act)
    return logistic * (1.0 + pre_act * (1.0 - logistic))


def swapped(value):
    return lax.ppermute(value, "tp", SWAP)


def selection(routes, route_weight, experts):
    rows = routes.shape[0]
    ids = lax.broadcasted_iota(jnp.int32, (experts, rows), 0)
    hits = [ids == routes[:, k][None, :] for k in range(routes.shape[1])]
    named = sum(h.astype(jnp.float32) for h in hits)
    weight = sum(
        jnp.where(h, route_weight[:, k][None, :], 0.0) for k, h in enumerate(hits)
    )
    earlier = lax.broadcasted_iota(jnp.int32, (rows, rows), 0) < lax.broadcasted_iota(
        jnp.int32, (rows, rows), 1
    )
    place = dot_f32(named.astype(jnp.bfloat16), earlier.astype(jnp.bfloat16), ((1,), (0,)))
    slot = lax.broadcasted_iota(jnp.int32, (experts, CAPACITY, rows), 1).astype(jnp.float32)
    chosen = (place[:, None, :] == slot) & (named[:, None, :] > 0.0)
    scale = jnp.sum(jnp.where(chosen, weight[:, None, :], 0.0), axis=2)
    matrix = chosen.astype(jnp.bfloat16).reshape(experts * CAPACITY, rows)
    return matrix, scale.reshape(experts * CAPACITY)


def per_device(
    mid_rows,
    cotangent,
    routes,
    route_weight,
    filtered,
    conv_taps,
    norm_gain,
    out_weight,
    gate_weight,
    up_weight,
    down_weight,
):
    sp_count = lax.axis_size(SP)
    width = mid_rows.shape[1]
    gate_mat, up_mat, down_mat = gate_weight[0], up_weight[0], down_weight[0]

    matrix, scale = selection(routes, route_weight, sp_count)
    inputs = dot_f32(matrix, mid_rows, ((1,), (0,))).astype(jnp.bfloat16)
    cot_rows = dot_f32(matrix, cotangent, ((1,), (0,)))
    routed = (scale[:, None] * cot_rows).astype(jnp.bfloat16)
    both = jnp.concatenate((inputs, routed), axis=1).reshape(sp_count, CAPACITY, 2 * width)
    arrived = lax.all_to_all(both, SP, split_axis=0, concat_axis=0, tiled=True)
    arrived = arrived.reshape(sp_count * CAPACITY, 2 * width)
    partner = swapped(arrived)
    all_rows = jnp.concatenate((partner, arrived), axis=0)
    all_in, all_cot = all_rows[:, :width], all_rows[:, width:]

    pre_gate = dot_f32(all_in, gate_mat, ((1,), (0,)))
    pre_up = dot_f32(all_in, up_mat, ((1,), (0,)))
    gate_act = jax.nn.silu(pre_gate)
    hidden = (gate_act * pre_up).astype(jnp.bfloat16)
    hidden_grad = dot_f32(all_cot, down_mat, ((1,), (1,)))
    gate_pre = (hidden_grad * pre_up * silu_grad(pre_gate)).astype(jnp.bfloat16)
    up_pre = (hidden_grad * gate_act).astype(jnp.bfloat16)
    half = sp_count * CAPACITY

    def part(rows):
        return (
            dot_f32(gate_pre[rows], gate_mat, ((1,), (1,)))
            + dot_f32(up_pre[rows], up_mat, ((1,), (1,)))
        ).astype(jnp.bfloat16)

    from_partner = swapped(part(slice(0, half)))
    kept = part(slice(half, 2 * half))
    back = (kept.astype(jnp.float32) + from_partner.astype(jnp.float32)).astype(jnp.bfloat16)
    returned = lax.all_to_all(
        back.reshape(sp_count, CAPACITY, width), SP, split_axis=0, concat_axis=0, tiled=True
    ).reshape(half, width)

    gate_grad = dot_f32(all_in, gate_pre, ((0,), (0,)))[None]
    up_grad = dot_f32(all_in, up_pre, ((0,), (0,)))[None]
    down_grad = dot_f32(hidden, all_cot, ((0,), (0,)))[None]

    route_sum = dot_f32(matrix, returned, ((0,), (0,)))
    mid_grad = (cotangent.astype(jnp.float32) + route_sum).astype(jnp.bfloat16)
    other = swapped(mid_grad)
    first = lax.axis_index("tp") == 0
    grad_tokens = jnp.concatenate(
        (jnp.where(first, mid_grad, other), jnp.where(first, other, mid_grad)), axis=0
    )

    values = filtered.astype(jnp.float32)
    sums = jnp.stack((jnp.sum(values, axis=1), jnp.sum(values * values, axis=1)))
    sums = sums + swapped(sums)
    average = sums[0] / width
    variance = sums[1] / width - average * average
    inv_scale = lax.rsqrt(variance + NORM_EPS)[:, None]
    normed = (values - average[:, None]) * inv_scale
    scaled = normed * norm_gain
    activated = jax.nn.silu(scaled).astype(jnp.bfloat16)

    partial = dot_f32(grad_tokens, activated, ((0,), (0,))).astype(jnp.bfloat16)
    pieces = lax.all_to_all(
        partial.reshape(sp_count, width // sp_count, partial.shape[1]),
        SP,
        split_axis=0,
        concat_axis=0,
        tiled=True,
    )
    proj_grad = jnp.sum(pieces.astype(jnp.float32), axis=0)

    act_grad = dot_f32(grad_tokens, out_weight, ((1,), (1,)))
    scaled_grad = act_grad * silu_grad(scaled) * norm_gain
    totals = jnp.stack((jnp.sum(scaled_grad, axis=1), jnp.sum(scaled_grad * normed, axis=1)))
    totals = totals + swapped(totals)
    grad_mean = (totals[0] / width)[:, None]
    grad_corr = (totals[1] / width)[:, None]
    conv_grad = (inv_scale * (scaled_grad - grad_mean - normed * grad_corr)).astype(jnp.bfloat16)

    taps = conv_taps.shape[0]
    reach = taps // 2
    rows = conv_grad.shape[0]
    low = lax.ppermute(
        conv_grad[rows - reach :], SP, [(i, i + 1) for i in range(sp_count - 1)]
    )
    high = lax.ppermute(conv_grad[:reach], SP, [(i + 1, i) for i in range(sp_count - 1)])
    padded = jnp.concatenate((low, conv_grad, high), axis=0)
    accumulated = jnp.zeros(conv_grad.shape, jnp.float32)
    for offset in range(taps):
        lead = 2 * reach - offset
        accumulated = accumulated + conv_taps[offset] * padded[lead : lead + rows]
    input_grad = accumulated.astype(jnp.bfloat16)
    return (gate_grad, up_grad, down_grad, proj_grad, input_grad)


def solution(mesh):
    split = Mesh(mesh.devices.reshape(4, 4, 4, mesh.shape["tp"]), ("sp_0", "sp_1", "sp_2", "tp"))
    in_specs = (
        P(SP_TP, None),
        P(SP_TP, None),
        P(SP_TP, None),
        P(SP_TP, None),
        P(SP, "tp"),
        P(None, "tp"),
        P("tp"),
        P("tp", None),
        P(SP, None, "tp"),
        P(SP, None, "tp"),
        P(SP, "tp", None),
    )
    out_specs = (P(SP, None, "tp"), P(SP, None, "tp"), P(SP, "tp", None), P(SP, "tp"), P(SP, "tp"))
    return jax.shard_map(
        per_device, mesh=split, in_specs=in_specs, out_specs=out_specs, check_vma=False
    )
```
